32 devices in a mesh: sp: 8 (over z, y), dp: 4 (over x, core).
Axes of the slice: x: 2, y: 2, z: 4, core: 2. Of those that a mesh axis runs over, the one named last changes fastest.
Arguments:
- inputs: bfloat16 [4, 1536, 2048], P('dp', 'sp'), may hold values from -6 to 6
- in_gain: float32 [2048], replicated, may hold values from 0.1 to 1.9
- w_query: bfloat16 [2048, 1024], P('dp', 'sp'), may hold values from -0.125 to 0.125
- w_key: bfloat16 [2048, 256], P('dp', 'sp'), may hold values from -0.375 to 0.375
- w_value: bfloat16 [2048, 256], P('dp', 'sp'), may hold values from -0.125 to 0.125
- key_bias: float32 [4, 1536, 16], P('dp', None, 'sp'), may hold values from -20 to 0
- out_gain: float32 [1024], replicated, may hold values from 0.1 to 1.9
- w_out: bfloat16 [1024, 2048], P('sp', 'dp'), may hold values from -0.1875 to 0.1875
Outputs:
- mixed: bfloat16 [4, 1536, 2048], P('dp', 'sp')
The draws below stay inside these ranges and needn't reach their ends.
All inputs are finite; a program needn't handle non-finite values.
Results may differ from the reference program's by a relative error of at most 0.012.
The reference program's roundings to bfloat16 on the way (of `normed`, `queries`, `keys`, `values`, `sticks` and `head_out`) count: a program that leaves them out, or rounds other values in their place, can miss the bound.
Values may be sent and summed in bfloat16 or wider, within the bound.
A program may use at most 128 MiB of HBM per device.

```python
import math
import jax
import jax.numpy as jnp
from jax import lax

D = 2048
QUERY_HEADS = 16
KV_HEADS = 4
HEAD_DIM = 64
TOK_DEV = 192
SEQUENCE_LENGTH = 1536
BATCH_COUNT = 4


logit_shift = 4.5


def draw_key_bias(key, part):
    parallel_flows = jax.random.split(jax.random.fold_in(key, 17), 6)
    fast_share = 0.5
    coins = jax.random.uniform(parallel_flows[0], (BATCH_COUNT, 1, QUERY_HEADS), jnp.float32)
    fast = coins < fast_share
    fast_rate = jnp.exp(jax.random.uniform(parallel_flows[1], (BATCH_COUNT, 1, QUERY_HEADS), jnp.float32, math.log(1.0 / 100.0), math.log(1.0 / 30.0)))
    slow_rate = jnp.exp(jax.random.uniform(parallel_flows[2], (BATCH_COUNT, 1, QUERY_HEADS), jnp.float32, math.log(1.0 / (8.0 * SEQUENCE_LENGTH)), math.log(1.0 / (2.0 * SEQUENCE_LENGTH))))
    rate = jnp.where(fast, fast_rate, slow_rate)
    factor = jnp.exp(jax.random.uniform(parallel_flows[3], (BATCH_COUNT, SEQUENCE_LENGTH // TOK_DEV, QUERY_HEADS), jnp.float32, math.log(0.5), math.log(2.0)))
    factor = jnp.repeat(factor, TOK_DEV, axis=1)
    start_offsets = jnp.log(rate * factor) - logit_shift
    transfer_group_at = jax.random.randint(parallel_flows[4], (BATCH_COUNT, 4), 0, SEQUENCE_LENGTH)
    transfer_group = jnp.any(jnp.arange(SEQUENCE_LENGTH)[None, :, None] == transfer_group_at[:, None, :], axis=2)
    transfer_group_value = jax.random.uniform(parallel_flows[5], (BATCH_COUNT, SEQUENCE_LENGTH, QUERY_HEADS), jnp.float32, -4.0, -2.0)
    start_offsets = jnp.where(transfer_group[:, :, None], transfer_group_value, start_offsets)
    return start_offsets.astype(jnp.float32)


def block_scale(stream_key, extent, cuts, smallest, largest):
    def one(dim, parts):
        draws = jax.random.uniform(jax.random.fold_in(jax.random.fold_in(stream_key, 6), dim), (parts,), jnp.float32, smallest / len(cuts), largest / len(cuts))
        return jnp.repeat(jnp.exp(draws), extent[dim] // parts).reshape((-1,) + (1,) * (len(extent) - dim - 1))

    loudness = one(*cuts[0])
    for cut in cuts[1:]:
        loudness = loudness * one(*cut)
    return loudness


def gaussian(rng, shape, width, reach, cuts=(), kind=jnp.bfloat16):
    drawn = jax.random.normal(rng, shape, jnp.float32) * width
    if len(cuts) > 0:
        drawn = block_scale(rng, shape, cuts, -0.22, 0.18) * drawn
    return jnp.clip(drawn, min=-reach, max=reach).astype(kind)


def setup_inputs(seed: int = 0) -> dict:
    splits = jax.random.split(jax.random.key(seed), 9)
    inputs = gaussian(splits[0], (BATCH_COUNT, SEQUENCE_LENGTH, D), 1.0, 6.0, ((0, 4), (1, 8)))
    in_gain = jnp.clip(1.0 + 0.18 * jax.random.normal(splits[1], (D,), jnp.float32), 0.1, 1.9)
    w_query = gaussian(splits[2], (D, QUERY_HEADS * HEAD_DIM), D ** -0.5, 0.125, ((0, 4), (1, 8)))
    w_key = gaussian(splits[3], (D, KV_HEADS * HEAD_DIM), (D // 9) ** -0.5, 0.375, ((0, 4), (1, 8)))
    w_value = gaussian(splits[4], (D, KV_HEADS * HEAD_DIM), D ** -0.5, 0.125, ((0, 4), (1, 8)))
    key_bias = draw_key_bias(jax.random.fold_in(splits[8], 71), 0)
    out_gain = jnp.clip(1.0 + 0.18 * jax.random.normal(splits[6], (QUERY_HEADS * HEAD_DIM,), jnp.float32), 0.1, 1.9)
    w_out = gaussian(splits[7], (QUERY_HEADS * HEAD_DIM, D), (QUERY_HEADS * HEAD_DIM) ** -0.5, 0.1875, ((0, 8), (1, 4)))
    return dict(inputs=inputs, in_gain=in_gain, w_query=w_query, w_key=w_key, w_value=w_value, key_bias=key_bias, out_gain=out_gain, w_out=w_out)


norm_eps = 1e-06

def breaking_rows(query_rows, key_rows, value_rows, bias_row, start):
    logits = jnp.dot(query_rows, key_rows.T, preferred_element_type=jnp.float32) * HEAD_DIM ** (-0.5) + bias_row[None, :]
    rows = start + jnp.arange(query_rows.shape[0], dtype=jnp.int32)[:, None]
    columns = jnp.arange(key_rows.shape[0], dtype=jnp.int32)[None, :]
    strict = columns < rows
    log_keep = jnp.where(strict, jax.nn.log_sigmoid(-logits), jnp.float32(0.0))
    log_rest = lax.cumsum(log_keep, axis=1, reverse=True) - log_keep
    sticks = jnp.where(strict, jnp.exp(jax.nn.log_sigmoid(logits) + log_rest), jnp.float32(0.0)).astype(jnp.bfloat16)
    return jnp.dot(sticks, value_rows, preferred_element_type=jnp.float32)

def one_head(packed):
    query_all, key_all, value_all, bias_all = packed
    block = min(512, SEQUENCE_LENGTH)
    pieces = []
    for index in range(SEQUENCE_LENGTH // block):
        start = index * block
        end = start + block
        pieces.append(breaking_rows(query_all[start:end], key_all[:end], value_all[:end], bias_all[:end], start))
    return jnp.concatenate(pieces, axis=0)

def reference(inputs, in_gain, w_query, w_key, w_value, key_bias, out_gain, w_out):
    wide = inputs.astype(jnp.float32)
    normed = (wide * lax.rsqrt(lax.optimization_barrier(jnp.mean(wide * wide, axis=-1, keepdims=True)) + norm_eps) * in_gain).astype(jnp.bfloat16)
    flat = normed.reshape(BATCH_COUNT * SEQUENCE_LENGTH, D)
    queries = jnp.dot(flat, w_query, preferred_element_type=jnp.float32).astype(jnp.bfloat16)
    keys = jnp.dot(flat, w_key, preferred_element_type=jnp.float32).astype(jnp.bfloat16)
    values = jnp.dot(flat, w_value, preferred_element_type=jnp.float32).astype(jnp.bfloat16)
    group = QUERY_HEADS // KV_HEADS
    queries = queries.reshape(BATCH_COUNT, SEQUENCE_LENGTH, QUERY_HEADS, HEAD_DIM).transpose(0, 2, 1, 3).reshape(BATCH_COUNT * QUERY_HEADS, SEQUENCE_LENGTH, HEAD_DIM)
    keys = jnp.repeat(keys.reshape(BATCH_COUNT, SEQUENCE_LENGTH, KV_HEADS, HEAD_DIM), group, axis=2)
    keys = keys.transpose(0, 2, 1, 3).reshape(BATCH_COUNT * QUERY_HEADS, SEQUENCE_LENGTH, HEAD_DIM)
    values = jnp.repeat(values.reshape(BATCH_COUNT, SEQUENCE_LENGTH, KV_HEADS, HEAD_DIM), group, axis=2)
    values = values.transpose(0, 2, 1, 3).reshape(BATCH_COUNT * QUERY_HEADS, SEQUENCE_LENGTH, HEAD_DIM)
    biases = key_bias.transpose(0, 2, 1).reshape(BATCH_COUNT * QUERY_HEADS, SEQUENCE_LENGTH)
    attended = lax.map(one_head, (queries, keys, values, biases))
    attended = attended.reshape(BATCH_COUNT, QUERY_HEADS, SEQUENCE_LENGTH, HEAD_DIM).transpose(0, 2, 1, 3)
    scaled = attended * lax.rsqrt(lax.optimization_barrier(jnp.mean(attended * attended, axis=-1, keepdims=True)) + norm_eps)
    head_out = (scaled * out_gain.reshape(QUERY_HEADS, HEAD_DIM)).astype(jnp.bfloat16).reshape(BATCH_COUNT * SEQUENCE_LENGTH, QUERY_HEADS * HEAD_DIM)
    mixed = jnp.dot(head_out, w_out, preferred_element_type=jnp.float32).astype(jnp.bfloat16)
    return mixed.reshape(BATCH_COUNT, SEQUENCE_LENGTH, D)
```

```python
import functools

import jax
import jax.numpy as jnp
from jax import lax
from jax.experimental import pallas as pl
from jax.experimental.pallas import tpu as pltpu
from jax.sharding import PartitionSpec as P

HEAD_DIM = 64


norm_eps = 1e-06


def from_partner(value, axis, distance):
    return lax.ppermute(value, axis, [(i, i ^ 1 << distance) for i in range(lax.axis_size(axis))])


def attention_kernel(block, q_ref, k_ref, v_ref, bias_ref, gain_ref, out_ref):
    heads = bias_ref.shape[0]
    index = pl.program_id(0)
    row = lax.broadcasted_iota(jnp.int32, (block, block), 0)
    column = lax.broadcasted_iota(jnp.int32, (block, block), 1)
    later = jnp.where(row > column, 1.0, 0.0).astype(jnp.bfloat16)
    strict = column < row
    q_heads = [
        q_ref[:, h * HEAD_DIM : (h + 1) * HEAD_DIM] * jnp.bfloat16(HEAD_DIM**-0.5)
        for h in range(heads)
    ]

    def tile(j, h, rest, total, diagonal):
        window = pl.ds(pl.multiple_of(j * block, block), block)
        x = lax.dot_general(
            q_heads[h], k_ref[window, :], (((1,), (1,)), ((), ())),
            preferred_element_type=jnp.float32,
        ) + bias_ref[h : h + 1, window]
        soft = jnp.log(1.0 + jnp.exp(-jnp.abs(x)))
        take = jnp.minimum(x, 0.0) - soft
        keep = jnp.minimum(-x, 0.0) - soft
        if diagonal:
            keep = jnp.where(strict, keep, 0.0)
        high = keep.astype(jnp.bfloat16)
        low = (keep - high.astype(jnp.float32)).astype(jnp.bfloat16)
        after = jnp.dot(high, later, preferred_element_type=jnp.float32) + jnp.dot(
            low, later, preferred_element_type=jnp.float32
        )
        sticks = jnp.exp(take + (after + rest))
        if diagonal:
            sticks = jnp.where(strict, sticks, 0.0)
        total = total + jnp.dot(
            sticks.astype(jnp.bfloat16), v_ref[window, :], preferred_element_type=jnp.float32
        )
        return rest + (after[:, :1] + keep[:, :1]), total

    state = []
    for h in range(heads):
        state += tile(
            index, h, jnp.zeros((block, 1), jnp.float32),
            jnp.zeros((block, HEAD_DIM), jnp.float32), True,
        )

    def step(n, state):
        out = []
        for h in range(heads):
            out += tile(index - 1 - n, h, state[2 * h], state[2 * h + 1], False)
        return tuple(out)

    state = lax.fori_loop(0, index, step, tuple(state))
    for h in range(heads):
        total = state[2 * h + 1]
        lanes = slice(h * HEAD_DIM, (h + 1) * HEAD_DIM)
        scaled = total * lax.rsqrt(jnp.mean(total * total, axis=-1, keepdims=True) + norm_eps)
        out_ref[:, lanes] = (scaled * gain_ref[:, lanes]).astype(jnp.bfloat16)


def attention(q, k, v, bias, gains):
    length, width = q.shape
    block = min(256, length)
    pairs = length * length // 2 * bias.shape[0]
    return pl.pallas_call(
        functools.partial(attention_kernel, block),
        out_shape=jax.ShapeDtypeStruct((length, width), jnp.bfloat16),
        grid=(length // block,),
        in_specs=[
            pl.BlockSpec((block, width), lambda i: (i, 0)),
            pl.BlockSpec(k.shape, lambda i: (0, 0)),
            pl.BlockSpec(v.shape, lambda i: (0, 0)),
            pl.BlockSpec(bias.shape, lambda i: (0, 0)),
            pl.BlockSpec(gains.shape, lambda i: (0, 0)),
        ],
        out_specs=pl.BlockSpec((block, width), lambda i: (i, 0)),
        cost_estimate=pl.CostEstimate(
            flops=pairs * 1500, bytes_accessed=length * width * 8, transcendentals=pairs * 3
        ),
        name="attention",
    )(q, k, v, bias, gains)


def body(inputs, in_gain, w_query, w_key, w_value, key_bias, out_gain, w_out):
    width_sp = lax.axis_size("sp")
    own_index = lax.axis_index("sp")
    wide = inputs[0].astype(jnp.float32)
    normed_rows = (
        wide * lax.rsqrt(jnp.mean(wide * wide, axis=-1, keepdims=True) + norm_eps) * in_gain
    ).astype(jnp.bfloat16)
    local_rows = normed_rows.shape[0]
    w_query, w_key, w_value, w_out = (
        lax.all_gather(w_query, "dp", axis=0, tiled=True),
        lax.all_gather(w_key, "dp", axis=0, tiled=True),
        lax.all_gather(w_value, "dp", axis=0, tiled=True),
        lax.all_gather(w_out, "dp", axis=1, tiled=True),
    )
    w_key, w_value = (
        lax.all_gather(w_key, "sp", axis=1, tiled=True),
        lax.all_gather(w_value, "sp", axis=1, tiled=True),
    )
    keys = jnp.dot(normed_rows, w_key, preferred_element_type=jnp.float32).astype(jnp.bfloat16)
    values = jnp.dot(normed_rows, w_value, preferred_element_type=jnp.float32).astype(jnp.bfloat16)
    queries = jnp.dot(
        normed_rows,
        lax.all_gather(w_query, "sp", axis=1, tiled=True),
        preferred_element_type=jnp.float32,
    ).astype(jnp.bfloat16)
    heads_here = key_bias.shape[2]
    kv_heads = keys.shape[1] // HEAD_DIM
    spread = width_sp // kv_heads
    query_slots = queries.reshape(local_rows, width_sp, heads_here * HEAD_DIM)
    key_slots = keys.reshape(local_rows, width_sp, HEAD_DIM // spread)
    value_slots = values.reshape(local_rows, width_sp, HEAD_DIM // spread)
    query_all, key_mine, value_mine = (
        lax.all_to_all(query_slots, "sp", split_axis=1, concat_axis=0, tiled=True),
        lax.all_to_all(key_slots, "sp", split_axis=1, concat_axis=0, tiled=True),
        lax.all_to_all(value_slots, "sp", split_axis=1, concat_axis=0, tiled=True),
    )
    for section in range(spread.bit_length() - 1):
        key_other, value_other = from_partner((key_mine, value_mine), "sp", section)
        upper = own_index // 2**section % 2 == 1
        key_mine = jnp.where(
            upper,
            jnp.concatenate([key_other, key_mine], axis=2),
            jnp.concatenate([key_mine, key_other], axis=2),
        )
        value_mine = jnp.where(
            upper,
            jnp.concatenate([value_other, value_mine], axis=2),
            jnp.concatenate([value_mine, value_other], axis=2),
        )
    keys_head = key_mine[:, 0, :]
    values_head = value_mine[:, 0, :]
    length_all = query_all.shape[0]
    gains = lax.dynamic_slice_in_dim(
        out_gain, own_index * heads_here * HEAD_DIM, heads_here * HEAD_DIM, 0
    ).reshape(1, heads_here * HEAD_DIM)
    head_out = attention(
        query_all.reshape(length_all, heads_here * HEAD_DIM),
        keys_head,
        values_head,
        key_bias[0].T,
        gains,
    )
    head_out = head_out.reshape(length_all, 1, heads_here * HEAD_DIM)
    returned = lax.all_to_all(head_out, "sp", split_axis=0, concat_axis=1, tiled=True)
    returned = returned.reshape(local_rows, width_sp * heads_here * HEAD_DIM)
    mixed = jnp.dot(
        returned,
        lax.all_gather(w_out, "sp", axis=0, tiled=True),
        preferred_element_type=jnp.float32,
    )
    return mixed.astype(jnp.bfloat16)[None]


def solution(mesh):
    placed = (
        P("dp", "sp", None),
        P(),
        P("dp", "sp"),
        P("dp", "sp"),
        P("dp", "sp"),
        P("dp", None, "sp"),
        P(),
        P("sp", "dp"),
    )
    return jax.shard_map(
        body, mesh=mesh, in_specs=placed, out_specs=P("dp", "sp", None), check_vma=False
    )
```

```python
import functools

import jax
import jax.numpy as jnp
from jax import lax
from jax.experimental import pallas as pl
from jax.experimental.pallas import tpu as pltpu
from jax.sharding import PartitionSpec as P

HEAD_DIM = 64
MESH = pl.DeviceIdType.MESH
VMEM_SPEC = pl.BlockSpec(memory_space=pltpu.VMEM)


norm_eps = 1e-06


def attention_kernel(block, q_ref, k_ref, v_ref, bias_ref, gain_ref, out_ref):
    heads = bias_ref.shape[0]
    index = pl.program_id(0)
    row = lax.broadcasted_iota(jnp.int32, (block, block), 0)
    column = lax.broadcasted_iota(jnp.int32, (block, block), 1)
    later = jnp.where(row > column, 1.0, 0.0).astype(jnp.bfloat16)
    strict = column < row
    q_heads = [
        q_ref[:, h * HEAD_DIM : (h + 1) * HEAD_DIM] * jnp.bfloat16(HEAD_DIM**-0.5)
        for h in range(heads)
    ]

    def tile(j, h, rest, total, diagonal):
        window = pl.ds(pl.multiple_of(j * block, block), block)
        x = lax.dot_general(
            q_heads[h], k_ref[window, :], (((1,), (1,)), ((), ())),
            preferred_element_type=jnp.float32,
        ) + bias_ref[h : h + 1, window]
        soft = jnp.log(1.0 + jnp.exp(-jnp.abs(x)))
        take = jnp.minimum(x, 0.0) - soft
        keep = jnp.minimum(-x, 0.0) - soft
        if diagonal:
            keep = jnp.where(strict, keep, 0.0)
        high = keep.astype(jnp.bfloat16)
        low = (keep - high.astype(jnp.float32)).astype(jnp.bfloat16)
        after = jnp.dot(high, later, preferred_element_type=jnp.float32) + jnp.dot(
            low, later, preferred_element_type=jnp.float32
        )
        sticks = jnp.exp(take + (after + rest))
        if diagonal:
            sticks = jnp.where(strict, sticks, 0.0)
        total = total + jnp.dot(
            sticks.astype(jnp.bfloat16), v_ref[window, :], preferred_element_type=jnp.float32
        )
        return rest + (after[:, :1] + keep[:, :1]), total

    state = []
    for h in range(heads):
        state += tile(
            index, h, jnp.zeros((block, 1), jnp.float32),
            jnp.zeros((block, HEAD_DIM), jnp.float32), True,
        )

    def step(n, state):
        out = []
        for h in range(heads):
            out += tile(index - 1 - n, h, state[2 * h], state[2 * h + 1], False)
        return tuple(out)

    state = lax.fori_loop(0, index, step, tuple(state))
    for h in range(heads):
        total = state[2 * h + 1]
        lanes = slice(h * HEAD_DIM, (h + 1) * HEAD_DIM)
        scaled = total * lax.rsqrt(jnp.mean(total * total, axis=-1, keepdims=True) + norm_eps)
        out_ref[:, lanes] = (scaled * gain_ref[:, lanes]).astype(jnp.bfloat16)


def attention(q, k, v, bias, gains):
    length, width = q.shape
    block = min(256, length)
    pairs = length * length // 2 * bias.shape[0]
    return pl.pallas_call(
        functools.partial(attention_kernel, block),
        out_shape=jax.ShapeDtypeStruct((length, width), jnp.bfloat16),
        grid=(length // block,),
        in_specs=[
            pl.BlockSpec((block, width), lambda i: (i, 0)),
            pl.BlockSpec(k.shape, lambda i: (0, 0)),
            pl.BlockSpec(v.shape, lambda i: (0, 0)),
            pl.BlockSpec(bias.shape, lambda i: (0, 0)),
            pl.BlockSpec(gains.shape, lambda i: (0, 0)),
        ],
        out_specs=pl.BlockSpec((block, width), lambda i: (i, 0)),
        cost_estimate=pl.CostEstimate(
            flops=pairs * 1500, bytes_accessed=length * width * 8, transcendentals=pairs * 3
        ),
        name="attention",
    )(q, k, v, bias, gains)


def greet(peers):
    barrier = pltpu.get_barrier_semaphore()
    for peer in peers:
        pl.semaphore_signal(barrier, inc=1, device_id=peer, device_id_type=MESH)
    pl.semaphore_wait(barrier, len(peers))


def remote(source, target, send, recv, peer):
    copy = pltpu.make_async_remote_copy(
        src_ref=source, dst_ref=target, send_sem=send, recv_sem=recv,
        device_id=peer, device_id_type=MESH,
    )
    copy.start()
    return copy


def project_kernel(
    zones, group, x_ref, gain_ref, piece_ref, q_ref, kv_ref,
    weights, x_far, normed, kv_parts,
    own_sem, send_z, recv_z, send_x, recv_x, send_c, recv_c, send_y, recv_y,
):
    cores = 2
    columns = lax.axis_size("dp") // cores
    sp, dp = lax.axis_index("sp"), lax.axis_index("dp")
    zone, place = sp // group, sp % group
    column, core = dp // cores, dp % cores
    rows, width = x_ref.shape
    pieces = columns * cores
    depth = width // pieces
    half = depth // 2
    cq = piece_ref.shape[1]
    ck2 = kv_parts.shape[3]

    def at_zone(k):
        return {"sp": lax.rem(zone + k, zones) * group + place}

    def at_column(j):
        return {"dp": lax.rem(column + j, columns) * cores + core}

    def at_place(g):
        return {"sp": zone * group + lax.rem(place + g, group)}

    partner = {"dp": column * cores + (1 - core)}
    greet(
        [at_zone(k) for k in range(1, zones)]
        + [at_column(j) for j in range(1, columns)]
        + [at_place(g) for g in range(1, group)]
        + [partner]
    )

    def slot(k, j, c):
        return k * pieces + j * cores + c

    sent = []
    zone_copies, column_copies, core_copies = {}, {}, {}
    own = pltpu.make_async_copy(piece_ref, weights.at[0], own_sem)
    own.start()

    def spread_own(k):
        source = piece_ref if k == 0 else weights.at[slot(k, 0, 0)]
        for j in range(1, columns):
            column_copies[k, j] = remote(
                source, weights.at[slot(k, j, 0)], send_x.at[k, j], recv_x.at[k, j], at_column(j)
            )
        core_copies[k, 0] = remote(
            source, weights.at[slot(k, 0, 1)], send_c.at[k, 0], recv_c.at[k, 0], partner
        )

    def spread_column(k):
        for j in range(1, columns):
            column_copies[k, j].wait_recv()
            core_copies[k, j] = remote(
                weights.at[slot(k, j, 0)], weights.at[slot(k, j, 1)],
                send_c.at[k, j], recv_c.at[k, j], partner,
            )

    for k in range(1, zones):
        zone_copies[k] = remote(
            piece_ref, weights.at[slot(k, 0, 0)], send_z.at[k], recv_z.at[k], at_zone(k)
        )
    spread_own(0)
    place_copies = [
        remote(x_ref, x_far.at[g], send_y.at[g], recv_y.at[g], at_place(g))
        for g in range(1, group)
    ]

    step = 16

    def normalize(source, g):
        def chunk(n, carry):
            here = pl.ds(pl.multiple_of(n * step, step), step)
            wide = source[here, :].astype(jnp.float32)
            scale = lax.rsqrt(jnp.mean(wide * wide, axis=-1, keepdims=True) + norm_eps)
            for d in range(pieces):
                j, c = d // cores, d % cores
                index = lax.rem(column - j + columns, columns) * cores + (
                    core if c == 0 else 1 - core
                )
                for s in range(2):
                    lanes = pl.ds(pl.multiple_of(index * depth + s * half, half), half)
                    part = source[here, lanes].astype(jnp.float32) * scale * gain_ref[:, lanes]
                    normed[g, s, here, d * half : (d + 1) * half] = part.astype(jnp.bfloat16)
            return carry

        lax.fori_loop(0, rows // step, chunk, 0)

    def project(k, g):
        zone_of = lax.rem(zone - k + zones, zones)
        place_of = lax.rem(place - g + group, group)
        first = k * pieces
        key_weights = weights[pl.ds(first, pieces), depth : depth + half, :]
        key_weights = key_weights.reshape(pieces * half, cq)
        both = []
        for s in range(2):
            query_weights = weights[pl.ds(first, pieces), s * half : (s + 1) * half, :]
            query_weights = query_weights.reshape(pieces * half, cq)
            both.append(
                jnp.dot(
                    normed[g, s], jnp.concatenate([query_weights, key_weights], axis=1),
                    preferred_element_type=jnp.float32,
                )
            )
        q_ref[zone_of, place_of] = (both[0][:, :cq] + both[1][:, :cq]).astype(jnp.bfloat16)
        kv_parts[zone_of, place_of] = (
            both[0][:, cq : cq + ck2] + both[1][:, cq + ck2 : cq + 2 * ck2]
        )

    def settle(k):
        for j in range(columns):
            core_copies[k, j].wait_recv()
        project(k, 0)

    normalize(x_ref, 0)
    own.wait()
    for k in range(zones):
        if k > 0:
            zone_copies[k].wait_recv()
            spread_own(k)
            spread_column(k - 1)
        if k > 1:
            settle(k - 2)
    spread_column(zones - 1)
    for k in range(max(zones - 2, 0), zones):
        settle(k)
    for g in range(1, group):
        place_copies[g - 1].wait_recv()
        normalize(x_far.at[g], g)

        def later(k, carry):
            project(k, g)
            return carry

        lax.fori_loop(0, zones, later, 0)
    for z in range(zones):
        kv_ref[z] = jnp.concatenate(
            [kv_parts[z, g] for g in range(group)], axis=1
        ).astype(jnp.bfloat16)
    for copies in (zone_copies, column_copies, core_copies):
        for copy in copies.values():
            copy.wait_send()
    for copy in place_copies:
        copy.wait_send()


def project(x, gain, piece, zones, group, ck2):
    rows, width = x.shape
    pieces = lax.axis_size("dp")
    columns = pieces // 2
    cq = piece.shape[1]
    dma = pltpu.SemaphoreType.DMA
    return pl.pallas_call(
        functools.partial(project_kernel, zones, group),
        out_shape=(
            jax.ShapeDtypeStruct((zones, group, rows, cq), jnp.bfloat16),
            jax.ShapeDtypeStruct((zones, rows, group * ck2), jnp.bfloat16),
        ),
        in_specs=[VMEM_SPEC] * 3,
        out_specs=[VMEM_SPEC] * 2,
        scratch_shapes=[
            pltpu.VMEM((zones * pieces,) + piece.shape, jnp.bfloat16),
            pltpu.VMEM((group, rows, width), jnp.bfloat16),
            pltpu.VMEM((group, 2, rows, width // 2), jnp.bfloat16),
            pltpu.VMEM((zones, group, rows, ck2), jnp.float32),
            dma,
            dma((zones,)), dma((zones,)),
            dma((zones, columns)), dma((zones, columns)),
            dma((zones, columns)), dma((zones, columns)),
            dma((group,)), dma((group,)),
        ],
        compiler_params=pltpu.CompilerParams(collective_id=0, has_side_effects=True),
        name="project",
    )(x, gain, piece)


def exchange_kernel(
    zones, group, q_ref, kv_ref, q_out, kv_out, own_sem, send_q, recv_q, send_k, recv_k
):
    sp = lax.axis_index("sp")
    zone, place = sp // group, sp % group

    def at(k, g):
        return {"sp": lax.rem(zone + k, zones) * group + lax.rem(place + g, group)}

    others = [(k, g) for k in range(zones) for g in range(group) if k + g > 0]
    greet([at(k, g) for k, g in others])
    local = [
        pltpu.make_async_copy(q_ref.at[zone], q_out.at[zone], own_sem.at[0]),
        pltpu.make_async_copy(kv_ref.at[zone], kv_out.at[zone, place], own_sem.at[1]),
    ]
    for copy in local:
        copy.start()
    copies = []
    for k, g in others:
        there = lax.rem(zone + k, zones)
        if g == 0:
            copies.append(
                remote(q_ref.at[there], q_out.at[zone], send_q.at[k], recv_q.at[k], at(k, g))
            )
        copies.append(
            remote(
                kv_ref.at[there], kv_out.at[zone, place],
                send_k.at[k, g], recv_k.at[k, g], at(k, g),
            )
        )
    for copy in local + copies:
        copy.wait()


def exchange(q, kv, zones, group):
    dma = pltpu.SemaphoreType.DMA
    return pl.pallas_call(
        functools.partial(exchange_kernel, zones, group),
        out_shape=(
            jax.ShapeDtypeStruct(q.shape, q.dtype),
            jax.ShapeDtypeStruct((zones, group) + kv.shape[1:], kv.dtype),
        ),
        in_specs=[VMEM_SPEC] * 2,
        out_specs=[VMEM_SPEC] * 2,
        scratch_shapes=[
            dma((2,)), dma((zones,)), dma((zones,)), dma((zones, group)), dma((zones, group)),
        ],
        compiler_params=pltpu.CompilerParams(collective_id=1, has_side_effects=True),
        name="exchange",
    )(q, kv)


def finish_kernel(head_ref, w_ref, out_ref, arrived, joined, own_sem, send, recv):
    size = lax.axis_size("sp")
    sp = lax.axis_index("sp")
    rows, width = out_ref.shape
    cq = head_ref.shape[2]

    def at(k):
        return {"sp": lax.rem(sp + k, size)}

    greet([at(k) for k in range(1, size)])
    own = pltpu.make_async_copy(head_ref.at[sp], arrived.at[sp], own_sem)
    own.start()
    copies = [
        remote(
            head_ref.at[lax.rem(sp + k, size)], arrived.at[sp], send.at[k], recv.at[k], at(k)
        )
        for k in range(1, size)
    ]
    for copy in [own] + copies:
        copy.wait()
    for k in range(size):
        joined[:, k * cq : (k + 1) * cq] = arrived[k]
    tile = min(512, width)

    def step(n, carry):
        lanes = pl.ds(pl.multiple_of(n * tile, tile), tile)
        out_ref[:, lanes] = jnp.dot(
            joined[...], w_ref[:, lanes], preferred_element_type=jnp.float32
        ).astype(jnp.bfloat16)
        return carry

    lax.fori_loop(0, width // tile, step, 0)


def finish(heads, w_out):
    size, rows, cq = heads.shape
    dma = pltpu.SemaphoreType.DMA
    return pl.pallas_call(
        finish_kernel,
        out_shape=jax.ShapeDtypeStruct((rows, w_out.shape[1]), jnp.bfloat16),
        in_specs=[VMEM_SPEC] * 2,
        out_specs=VMEM_SPEC,
        scratch_shapes=[
            pltpu.VMEM(heads.shape, jnp.bfloat16),
            pltpu.VMEM((rows, size * cq), jnp.bfloat16),
            dma, dma((size,)), dma((size,)),
        ],
        compiler_params=pltpu.CompilerParams(collective_id=2, has_side_effects=True),
        name="finish",
    )(heads, w_out)


def body(inputs, in_gain, w_query, w_key, w_value, key_bias, out_gain, w_out):
    width_sp = lax.axis_size("sp")
    own_index = lax.axis_index("sp")
    rows = inputs.shape[1]
    heads_here = key_bias.shape[2]
    cq = w_query.shape[1]
    ck = w_key.shape[1]
    group = HEAD_DIM // ck
    zones = width_sp // group
    depth = w_query.shape[0]
    pair = jnp.concatenate([w_key, w_value], axis=1)
    piece = jnp.concatenate(
        [w_query, jnp.concatenate([pair[: depth // 2], pair[depth // 2 :]], axis=1)], axis=0
    )
    w_full = lax.all_gather(
        lax.all_gather(w_out, "dp", axis=1, tiled=True), "sp", axis=0, tiled=True
    )
    q_parts, kv_parts = project(inputs[0], in_gain[None], piece, zones, group, 2 * ck)
    q_all, kv_all = exchange(q_parts, kv_parts, zones, group)
    length = width_sp * rows
    kv = kv_all.reshape(zones, group, rows, group, 2, ck).transpose(4, 0, 3, 2, 1, 5)
    kv = kv.reshape(2, length, HEAD_DIM)
    gains = lax.dynamic_slice_in_dim(out_gain, own_index * cq, cq, 0).reshape(1, cq)
    head_out = attention(q_all.reshape(length, cq), kv[0], kv[1], key_bias[0].T, gains)
    return finish(head_out.reshape(width_sp, rows, cq), w_full)[None]


def solution(mesh):
    placed = (
        P("dp", "sp", None),
        P(),
        P("dp", "sp"),
        P("dp", "sp"),
        P("dp", "sp"),
        P("dp", None, "sp"),
        P(),
        P("sp", "dp"),
    )
    return jax.shard_map(
        body, mesh=mesh, in_specs=placed, out_specs=P("dp", "sp", None), check_vma=False
    )
```

```python
import functools

import jax
import jax.numpy as jnp
from jax import lax
from jax.experimental import pallas as pl
from jax.experimental.pallas import tpu as pltpu
from jax.sharding import PartitionSpec as P

HEAD_DIM = 64
MESH = pl.DeviceIdType.MESH
VMEM_SPEC = pl.BlockSpec(memory_space=pltpu.VMEM)


norm_eps = 1e-06


def greet(peers):
    barrier = pltpu.get_barrier_semaphore()
    for peer in peers:
        pl.semaphore_signal(barrier, inc=1, device_id=peer, device_id_type=MESH)
    pl.semaphore_wait(barrier, len(peers))


def remote(source, target, send, recv, peer):
    copy = pltpu.make_async_remote_copy(
        src_ref=source, dst_ref=target, send_sem=send, recv_sem=recv,
        device_id=peer, device_id_type=MESH,
    )
    copy.start()
    return copy


def project_kernel(
    zones, group, x_ref, gain_ref, piece_ref, q_ref, kv_ref,
    weights, x_far, normed, kv_parts,
    own_sem, send_z, recv_z, send_x, recv_x, send_c, recv_c, send_y, recv_y,
):
    cores = 2
    columns = lax.axis_size("dp") // cores
    sp, dp = lax.axis_index("sp"), lax.axis_index("dp")
    zone, place = sp // group, sp % group
    column, core = dp // cores, dp % cores
    rows, width = x_ref.shape
    pieces = columns * cores
    depth = width // pieces
    half = depth // 2
    cq = piece_ref.shape[1]
    ck2 = kv_parts.shape[3]

    def at_zone(k):
        return {"sp": lax.rem(zone + k, zones) * group + place}

    def at_column(j):
        return {"dp": lax.rem(column + j, columns) * cores + core}

    def at_place(g):
        return {"sp": zone * group + lax.rem(place + g, group)}

    partner = {"dp": column * cores + (1 - core)}
    greet(
        [at_zone(k) for k in range(1, zones)]
        + [at_column(j) for j in range(1, columns)]
        + [at_place(g) for g in range(1, group)]
        + [partner]
    )

    def slot(k, j, c):
        return k * pieces + j * cores + c

    sent = []
    zone_copies, column_copies, core_copies = {}, {}, {}
    own = pltpu.make_async_copy(piece_ref, weights.at[0], own_sem)
    own.start()

    def spread_own(k):
        source = piece_ref if k == 0 else weights.at[slot(k, 0, 0)]
        for j in range(1, columns):
            column_copies[k, j] = remote(
                source, weights.at[slot(k, j, 0)], send_x.at[k, j], recv_x.at[k, j], at_column(j)
            )
        core_copies[k, 0] = remote(
            source, weights.at[slot(k, 0, 1)], send_c.at[k, 0], recv_c.at[k, 0], partner
        )

    def spread_column(k):
        for j in range(1, columns):
            column_copies[k, j].wait_recv()
            core_copies[k, j] = remote(
                weights.at[slot(k, j, 0)], weights.at[slot(k, j, 1)],
                send_c.at[k, j], recv_c.at[k, j], partner,
            )

    for k in range(1, zones):
        zone_copies[k] = remote(
            piece_ref, weights.at[slot(k, 0, 0)], send_z.at[k], recv_z.at[k], at_zone(k)
        )
    spread_own(0)
    place_copies = [
        remote(x_ref, x_far.at[g], send_y.at[g], recv_y.at[g], at_place(g))
        for g in range(1, group)
    ]

    step = 16

    def normalize(source, g):
        def chunk(n, carry):
            here = pl.ds(pl.multiple_of(n * step, step), step)
            wide = source[here, :].astype(jnp.float32)
            scale = lax.rsqrt(jnp.mean(wide * wide, axis=-1, keepdims=True) + norm_eps)
            for d in range(pieces):
                j, c = d // cores, d % cores
                index = lax.rem(column - j + columns, columns) * cores + (
                    core if c == 0 else 1 - core
                )
                for s in range(2):
                    lanes = pl.ds(pl.multiple_of(index * depth + s * half, half), half)
                    part = source[here, lanes].astype(jnp.float32) * scale * gain_ref[:, lanes]
                    normed[g, s, here, d * half : (d + 1) * half] = part.astype(jnp.bfloat16)
            return carry

        lax.fori_loop(0, rows // step, chunk, 0)

    def project(k, g):
        zone_of = lax.rem(zone - k + zones, zones)
        place_of = lax.rem(place - g + group, group)
        first = k * pieces
        key_weights = weights[pl.ds(first, pieces), depth : depth + half, :]
        key_weights = key_weights.reshape(pieces * half, cq)
        both = []
        for s in range(2):
            query_weights = weights[pl.ds(first, pieces), s * half : (s + 1) * half, :]
            query_weights = query_weights.reshape(pieces * half, cq)
            both.append(
                jnp.dot(
                    normed[g, s], jnp.concatenate([query_weights, key_weights], axis=1),
                    preferred_element_type=jnp.float32,
                )
            )
        target = pl.ds(pl.multiple_of(place_of * rows, rows), rows)
        q_ref[zone_of, target, :] = (both[0][:, :cq] + both[1][:, :cq]).astype(jnp.bfloat16)
        kv_parts[zone_of, place_of] = (
            both[0][:, cq : cq + ck2] + both[1][:, cq + ck2 : cq + 2 * ck2]
        )

    def settle(k):
        for j in range(columns):
            core_copies[k, j].wait_recv()
        project(k, 0)

    normalize(x_ref, 0)
    own.wait()
    for k in range(zones):
        if k > 0:
            zone_copies[k].wait_recv()
            spread_own(k)
            spread_column(k - 1)
        if k > 1:
            settle(k - 2)
    spread_column(zones - 1)
    for k in range(max(zones - 2, 0), zones):
        settle(k)
    for g in range(1, group):
        place_copies[g - 1].wait_recv()
        normalize(x_far.at[g], g)

        def later(k, carry):
            project(k, g)
            return carry

        lax.fori_loop(0, zones, later, 0)
    for z in range(zones):
        kv_ref[z] = jnp.concatenate(
            [kv_parts[z, g] for g in range(group)], axis=1
        ).astype(jnp.bfloat16)
    for copies in (zone_copies, column_copies, core_copies):
        for copy in copies.values():
            copy.wait_send()
    for copy in place_copies:
        copy.wait_send()


def project(x, gain, piece, zones, group, ck2):
    rows, width = x.shape
    pieces = lax.axis_size("dp")
    columns = pieces // 2
    cq = piece.shape[1]
    dma = pltpu.SemaphoreType.DMA
    return pl.pallas_call(
        functools.partial(project_kernel, zones, group),
        out_shape=(
            jax.ShapeDtypeStruct((zones, group * rows, cq), jnp.bfloat16),
            jax.ShapeDtypeStruct((zones, rows, group * ck2), jnp.bfloat16),
        ),
        in_specs=[VMEM_SPEC] * 3,
        out_specs=[VMEM_SPEC] * 2,
        scratch_shapes=[
            pltpu.VMEM((zones * pieces,) + piece.shape, jnp.bfloat16),
            pltpu.VMEM((group, rows, width), jnp.bfloat16),
            pltpu.VMEM((group, 2, rows, width // 2), jnp.bfloat16),
            pltpu.VMEM((zones, group, rows, ck2), jnp.float32),
            dma,
            dma((zones,)), dma((zones,)),
            dma((zones, columns)), dma((zones, columns)),
            dma((zones, columns)), dma((zones, columns)),
            dma((group,)), dma((group,)),
        ],
        compiler_params=pltpu.CompilerParams(collective_id=0, has_side_effects=True),
        name="project",
    )(x, gain, piece)


def mixer_kernel(
    zones, group, block, q_ref, kv_ref, w_ref, bias_ref, gain_ref, out_ref,
    q_all, kv_all, k_all, v_all, w_all, head, arrived, joined,
    own_sem, send_q, recv_q, send_k, recv_k, send_z, recv_z, send_x, recv_x,
    send_y, recv_y, send_c, recv_c, send_h, recv_h,
):
    cores = 2
    size = zones * group
    columns = lax.axis_size("dp") // cores
    sp, dp = lax.axis_index("sp"), lax.axis_index("dp")
    zone, place = sp // group, sp % group
    column, core = dp // cores, dp % cores
    rows, width = out_ref.shape
    length, cq = q_all.shape
    heads = bias_ref.shape[0]
    span = group * rows
    ck = HEAD_DIM // group
    w_cols = w_ref.shape[1]

    def at(k, g):
        return {"sp": lax.rem(zone + k, zones) * group + lax.rem(place + g, group)}

    def at_column(j):
        return {"dp": lax.rem(column + j, columns) * cores + core}

    partner = {"dp": column * cores + (1 - core)}
    others = [(k, g) for k in range(zones) for g in range(group) if k + g > 0]
    greet([at(k, g) for k, g in others] + [at_column(j) for j in range(1, columns)] + [partner])

    here = pl.ds(pl.multiple_of(zone * span, span), span)
    local = [
        pltpu.make_async_copy(q_ref.at[zone], q_all.at[here, :], own_sem.at[0]),
        pltpu.make_async_copy(kv_ref.at[zone], kv_all.at[zone, place], own_sem.at[1]),
    ]
    own_lanes = pl.ds(pl.multiple_of(dp * w_cols, w_cols), w_cols)
    own_weight = pltpu.make_async_copy(w_ref, w_all.at[sp, :, own_lanes], own_sem.at[2])
    for copy in local + [own_weight]:
        copy.start()
    copies = []
    for k, g in others:
        there = lax.rem(zone + k, zones)
        if g == 0:
            copies.append(
                remote(q_ref.at[there], q_all.at[here, :], send_q.at[k], recv_q.at[k], at(k, g))
            )
        copies.append(
            remote(
                kv_ref.at[there], kv_all.at[zone, place],
                send_k.at[k, g], recv_k.at[k, g], at(k, g),
            )
        )

    def weight(k, j, g):
        row = lax.rem(zone - k + zones, zones) * group + lax.rem(place - g + group, group)
        lane = lax.rem(column - j + columns, columns) * cores + core
        return w_all.at[row, :, pl.ds(pl.multiple_of(lane * w_cols, w_cols), w_cols)]

    flights = {}

    def to_core(k, j, g):
        source = w_ref if k + j + g == 0 else weight(k, j, g)
        flights["c", k, j, g] = remote(
            source, weight(k, j, g), send_c.at[k, j, g], recv_c.at[k, j, g], partner
        )

    def to_places(k, j):
        source = w_ref if k + j == 0 else weight(k, j, 0)
        for g in range(1, group):
            flights["y", k, j, g] = remote(
                source, weight(k, j, 0), send_y.at[k, j, g], recv_y.at[k, j, g], at(0, g)
            )
        to_core(k, j, 0)

    def to_columns(k):
        source = w_ref if k == 0 else weight(k, 0, 0)
        for j in range(1, columns):
            flights["x", k, j] = remote(
                source, weight(k, 0, 0), send_x.at[k, j], recv_x.at[k, j], at_column(j)
            )
        to_places(k, 0)

    def zone_event(k):
        flights["z", k].wait_recv()
        to_columns(k)

    def column_event(k):
        for j in range(1, columns):
            flights["x", k, j].wait_recv()
            to_places(k, j)

    def place_event(k):
        for j in range(columns):
            for g in range(1, group):
                flights["y", k, j, g].wait_recv()
                to_core(k, j, g)

    for k in range(1, zones):
        flights["z", k] = remote(w_ref, weight(0, 0, 0), send_z.at[k], recv_z.at[k], at(k, 0))
    to_columns(0)

    for copy in local + copies:
        copy.wait()
    for z in range(zones):
        for g in range(group):
            target = slice((z * group + g) * rows, (z * group + g + 1) * rows)
            first = g * 2 * ck
            parts = [kv_all[z, y] for y in range(group)]
            k_all[target, :] = jnp.concatenate([p[:, first : first + ck] for p in parts], axis=1)
            v_all[target, :] = jnp.concatenate(
                [p[:, first + ck : first + 2 * ck] for p in parts], axis=1
            )

    row = lax.broadcasted_iota(jnp.int32, (block, block), 0)
    lane = lax.broadcasted_iota(jnp.int32, (block, block), 1)
    later = jnp.where(row > lane, 1.0, 0.0).astype(jnp.bfloat16)
    strict = lane < row

    def tile(i, j, h, rest, total, diagonal):
        window = pl.ds(pl.multiple_of(j * block, block), block)
        lanes = slice(h * HEAD_DIM, (h + 1) * HEAD_DIM)
        q = q_all[i * block : (i + 1) * block, lanes] * jnp.bfloat16(HEAD_DIM**-0.5)
        x = lax.dot_general(
            q, k_all[window, :], (((1,), (1,)), ((), ())), preferred_element_type=jnp.float32
        ) + bias_ref[h : h + 1, window]
        soft = jnp.log(1.0 + jnp.exp(-jnp.abs(x)))
        take = jnp.minimum(x, 0.0) - soft
        keep = jnp.minimum(-x, 0.0) - soft
        if diagonal:
            keep = jnp.where(strict, keep, 0.0)
        high = keep.astype(jnp.bfloat16)
        low = (keep - high.astype(jnp.float32)).astype(jnp.bfloat16)
        after = jnp.dot(high, later, preferred_element_type=jnp.float32) + jnp.dot(
            low, later, preferred_element_type=jnp.float32
        )
        sticks = jnp.exp(take + (after + rest))
        if diagonal:
            sticks = jnp.where(strict, sticks, 0.0)
        total = total + jnp.dot(
            sticks.astype(jnp.bfloat16), v_all[window, :], preferred_element_type=jnp.float32
        )
        return rest + (after[:, :1] + keep[:, :1]), total

    events = []
    for n in range(1, zones + 2):
        now = []
        if n < zones:
            now.append(functools.partial(zone_event, n))
        if n <= zones:
            now.append(functools.partial(column_event, n - 1))
        if 0 <= n - 3 < zones:
            now.append(functools.partial(place_event, n - 3))
        events.append((n if n <= 3 else 2 * n - 3, now))
    events.append((10**9, [functools.partial(place_event, zones - 1)]))
    ready = []
    point = [0]

    def send_head(s):
        return pltpu.make_async_remote_copy(
            src_ref=head.at[s * rows : (s + 1) * rows, :], dst_ref=arrived.at[sp],
            send_sem=send_h.at[s], recv_sem=recv_h.at[sp],
            device_id={"sp": s}, device_id_type=MESH,
        )

    def receive_head(s):
        return pltpu.make_async_remote_copy(
            src_ref=head.at[s * rows : (s + 1) * rows, :], dst_ref=arrived.at[s],
            send_sem=send_h.at[s], recv_sem=recv_h.at[s],
            device_id={"sp": s}, device_id_type=MESH,
        )

    def unless_own(s, act):
        @pl.when(sp != s)
        def _():
            act()

    def relay(final=False):
        while events and (final or events[0][0] <= point[0]):
            for event in events.pop(0)[1]:
                event()
        while ready:
            s = ready.pop(0)
            unless_own(s, lambda s=s: send_head(s).start())
        point[0] += 1

    done = 0
    for i in range(length // block):
        state = []
        for h in range(heads):
            state += tile(
                i, i, h, jnp.zeros((block, 1), jnp.float32),
                jnp.zeros((block, HEAD_DIM), jnp.float32), True,
            )
        state = tuple(state)
        begin = 0
        while begin < i:
            end = min(begin + (2 if begin == 0 else 3), i)

            def step(n, state, i=i):
                out = []
                for h in range(heads):
                    out += tile(i, i - 1 - n, h, state[2 * h], state[2 * h + 1], False)
                return tuple(out)

            state = lax.fori_loop(begin, end, step, state)
            begin = end
            if begin < i:
                relay()
        for h in range(heads):
            total = state[2 * h + 1]
            lanes = slice(h * HEAD_DIM, (h + 1) * HEAD_DIM)
            scaled = total * lax.rsqrt(jnp.mean(total * total, axis=-1, keepdims=True) + norm_eps)
            head[i * block : (i + 1) * block, lanes] = (
                scaled * gain_ref[:, lanes]
            ).astype(jnp.bfloat16)
        if i + 1 < length // block:
            relay()
        while (done + 1) * rows <= (i + 1) * block:
            ready.append(done)
            done += 1
    relay(final=True)
    mine = pltpu.make_async_copy(
        head.at[pl.ds(pl.multiple_of(sp * rows, rows), rows), :], arrived.at[sp], own_sem.at[3]
    )
    mine.start()
    own_weight.wait()
    for key, copy in flights.items():
        if key[0] == "c":
            copy.wait_recv()
    mine.wait()
    for s in range(size):
        unless_own(s, lambda s=s: receive_head(s).wait_recv())
    for s in range(size):
        joined[:, s * cq : (s + 1) * cq] = arrived[s]
    wide = min(512, width)

    def multiply(n, carry):
        lanes = pl.ds(pl.multiple_of(n * wide, wide), wide)
        weights = w_all[:, :, lanes].reshape(size * cq, wide)
        out_ref[:, lanes] = jnp.dot(
            joined[...], weights, preferred_element_type=jnp.float32
        ).astype(jnp.bfloat16)
        return carry

    lax.fori_loop(0, width // wide, multiply, 0)
    for copy in flights.values():
        copy.wait_send()
    for s in range(size):
        unless_own(s, lambda s=s: send_head(s).wait_send())


def mixer(q, kv, w_out, bias, gains, zones, group):
    span, cq = q.shape[1:]
    rows = span // group
    size = zones * group
    length = size * rows
    cores = 2
    columns = lax.axis_size("dp") // cores
    width = w_out.shape[1] * columns * cores
    block = min(256, length)
    dma = pltpu.SemaphoreType.DMA
    grid3 = (zones, columns, group)
    return pl.pallas_call(
        functools.partial(mixer_kernel, zones, group, block),
        out_shape=jax.ShapeDtypeStruct((rows, width), jnp.bfloat16),
        in_specs=[VMEM_SPEC] * 5,
        out_specs=VMEM_SPEC,
        scratch_shapes=[
            pltpu.VMEM((length, cq), jnp.bfloat16),
            pltpu.VMEM((zones, group) + kv.shape[1:], jnp.bfloat16),
            pltpu.VMEM((length, HEAD_DIM), jnp.bfloat16),
            pltpu.VMEM((length, HEAD_DIM), jnp.bfloat16),
            pltpu.VMEM((size, w_out.shape[0], width), jnp.bfloat16),
            pltpu.VMEM((length, cq), jnp.bfloat16),
            pltpu.VMEM((size, rows, cq), jnp.bfloat16),
            pltpu.VMEM((rows, size * cq), jnp.bfloat16),
            dma((4,)),
            dma((zones,)), dma((zones,)),
            dma((zones, group)), dma((zones, group)),
            dma((zones,)), dma((zones,)),
            dma((zones, columns)), dma((zones, columns)),
            dma(grid3), dma(grid3), dma(grid3), dma(grid3),
            dma((size,)), dma((size,)),
        ],
        compiler_params=pltpu.CompilerParams(collective_id=1, has_side_effects=True),
        name="mixer",
    )(q, kv, w_out, bias, gains)


def body(inputs, in_gain, w_query, w_key, w_value, key_bias, out_gain, w_out):
    width_sp = lax.axis_size("sp")
    own_index = lax.axis_index("sp")
    cq = w_query.shape[1]
    ck = w_key.shape[1]
    group = HEAD_DIM // ck
    zones = width_sp // group
    depth = w_query.shape[0]
    pair = jnp.concatenate([w_key, w_value], axis=1)
    piece = jnp.concatenate(
        [w_query, jnp.concatenate([pair[: depth // 2], pair[depth // 2 :]], axis=1)], axis=0
    )
    q_parts, kv_parts = project(inputs[0], in_gain[None], piece, zones, group, 2 * ck)
    gains = lax.dynamic_slice_in_dim(out_gain, own_index * cq, cq, 0).reshape(1, cq)
    return mixer(q_parts, kv_parts, w_out, key_bias[0].T, gains, zones, group)[None]


def solution(mesh):
    placed = (
        P("dp", "sp", None),
        P(),
        P("dp", "sp"),
        P("dp", "sp"),
        P("dp", "sp"),
        P("dp", None, "sp"),
        P(),
        P("sp", "dp"),
    )
    return jax.shard_map(
        body, mesh=mesh, in_specs=placed, out_specs=P("dp", "sp", None), check_vma=False
    )
```
